32 devices in a mesh: fs: 4 (over y, x), tp: 8 (over z, core).
Axes of the slice: x: 2, y: 2, z: 4, core: 2. Of those that a mesh axis runs over, the one named last changes fastest.
Arguments:
- tokens: bfloat16 [2048, 2048], P('fs', 'tp'), may hold values from -6 to 6
- norm_gain: float32 [2048], P('fs'), may hold values from 0.1 to 1.9
- gate_train: float32 [2048, 8192], P('fs', 'tp'), may hold values from -0.125 to 0.125
- up_train: float32 [2048, 8192], P('fs', 'tp'), may hold values from -0.125 to 0.125
- down_train: float32 [8192, 2048], P('fs', 'tp'), may hold values from -0.0625 to 0.0625
Outputs:
- gate_serve: bfloat16 [2048, 8192], P(None, 'tp')
- up_serve: bfloat16 [2048, 8192], P(None, 'tp')
- down_serve: bfloat16 [8192, 2048], P('tp')
- layer_out: bfloat16 [2048, 2048], P(('fs', 'tp'))
The draws below stay inside these ranges and needn't reach their ends.
All inputs are finite; a program needn't handle non-finite values.
Results may differ from the reference program's by a relative error of at most 0.024.
Values may be sent and summed in bfloat16 or wider, within the bound.
A program may use at most 64 MiB of HBM per device.

```python
import jax
import jax.numpy as jnp
from jax import lax

D = 2048
FF = 8192
TOKENS = 2048


def level_of(own_key, shape, pieces, low, top_value):
    level, own = 1.0, jax.random.fold_in(own_key, 6)
    for position, parts in pieces:
        steps = jnp.exp(jax.random.uniform(jax.random.fold_in(own, position), (parts,), jnp.float32, low / len(pieces), top_value / len(pieces)))
        level = level * jnp.repeat(steps, shape[position] // parts).reshape([-1 if axis == position else 1 for axis in range(len(shape))])
    return level


def centred(own_key, extent, deviation, limit, shards=(), held_as=jnp.bfloat16):
    loudness = level_of(own_key, extent, shards, -0.22, 0.18) if shards else 1.0
    result = jax.random.normal(own_key, extent, jnp.float32) * deviation * loudness
    return jnp.minimum(jnp.maximum(result, -limit), limit).astype(held_as)


def setup_inputs(seed: int = 0) -> dict:
    splits = jax.random.split(jax.random.key(seed), 6)
    tokens = centred(splits[0], (TOKENS, D), 1.0, 6.0, ((0, 4), (1, 8)))
    norm_gain = jnp.clip(1.0 + 0.18 * jax.random.normal(splits[1], (D,), jnp.float32), 0.1, 1.9)
    gate_train = centred(splits[2], (D, FF), D ** -0.5, 0.125, ((0, 4), (1, 8)), jnp.float32)
    up_train = centred(splits[3], (D, FF), D ** -0.5, 0.125, ((0, 4), (1, 8)), jnp.float32)
    down_train = centred(splits[4], (FF, D), FF ** -0.5, 0.0625, ((0, 4), (1, 8)), jnp.float32)
    return dict(tokens=tokens, norm_gain=norm_gain, gate_train=gate_train, up_train=up_train, down_train=down_train)


def reference(tokens, norm_gain, gate_train, up_train, down_train):
    gate_serve = (norm_gain[:, None] * gate_train).astype(jnp.bfloat16)
    up_serve = (norm_gain[:, None] * up_train).astype(jnp.bfloat16)
    down_serve = down_train.astype(jnp.bfloat16)
    wide = tokens.astype(jnp.float32)
    scale = lax.rsqrt(lax.optimization_barrier(jnp.sum(wide * wide, axis=1)) / D + 1e-06)[:, None]
    gate = jnp.dot(tokens, gate_serve, preferred_element_type=jnp.float32)
    up_part = jnp.dot(tokens, up_serve, preferred_element_type=jnp.float32)
    hidden = (jax.nn.silu(gate * scale) * (up_part * scale)).astype(jnp.bfloat16)
    layer_out = jnp.dot(hidden, down_serve, preferred_element_type=jnp.float32).astype(jnp.bfloat16)
    return (gate_serve, up_serve, down_serve, layer_out)
```

```python
import functools

import jax
import jax.numpy as jnp
from jax import lax
from jax.experimental import pallas as pl
from jax.experimental.pallas import tpu as pltpu
from jax.sharding import PartitionSpec as P

MESH = pl.DeviceIdType.MESH
BF16 = jnp.bfloat16
F32 = jnp.float32
epsilon = 1e-06
CHUNKS = 4
X_ORDER = (0, 1, 2, 3)
Y_ORDER = (2, 3, 0, 1)


def flip(a, k):
    result = 0
    for bit in (1, 2, 4):
        own, other = (a // bit) % 2, (k // bit) % 2
        result = result + bit * (own + other - 2 * own * other)
    return result


def kernel(
    tok_in, gain_in, gate_in, up_in, down_in,
    gate_out, up_out, down_out, layer_out,
    w32, d32, wbuf, dcast, dbuf, tbuf, acc, hidden, scale, keep, psend, precv, zsend, zrecv,
    load_w, load_d, tok_s, tok_r, own_s, fwd_s, w_r, dz_s, d_s, d_r, out_w, out_d, p_s, p_r, z_s, z_r,
):
    f, t = lax.axis_index("fs"), lax.axis_index("tp")
    n_tp, n_fs = tbuf.shape[0], wbuf.shape[1]
    z, core = t // 2, t % 2
    fx, fy, fd = flip(f, 1), flip(f, 2), flip(f, 3)
    mate = flip(t, 1)
    rows = wbuf.shape[2]
    part = rows // CHUNKS
    w_ins, w_outs = (gate_in, up_in), (gate_out, up_out)
    tall, width = dbuf.shape[1], dbuf.shape[2]
    half = tall // 2
    per = n_tp // n_fs
    n_tok = tbuf.shape[1]
    piece_rows = n_tok // n_tp

    def remote(src, dst, ss, rs, to_f, to_t):
        return pltpu.make_async_remote_copy(
            src_ref=src, dst_ref=dst, send_sem=ss, recv_sem=rs, device_id=(to_f, to_t), device_id_type=MESH
        )

    def load(w, i):
        return pltpu.make_async_copy(w_ins[w].at[pl.ds(i * part, part)], w32.at[w, pl.ds(i * part, part)], load_w.at[w, i])

    order = (0, 2, 1, 3)
    for i in order:
        for w in range(2):
            load(w, i).start()
    load_down = [
        pltpu.make_async_copy(down_in.at[pl.ds(c * tall, tall)], d32.at[pl.ds(c * tall, tall)], load_d.at[c])
        for c in range(per)
    ]
    for copy in load_down:
        copy.start()

    barrier = pltpu.get_barrier_semaphore()
    peers = [(fx, t), (fy, t)] + [(f, flip(t, k)) for k in range(1, n_tp)]
    for peer in peers:
        pl.semaphore_signal(barrier, inc=1, device_id=peer, device_id_type=MESH)

    tbuf[t] = tok_in[...]

    def cast(w, i):
        block = pl.ds(i * part, part)
        load(w, i).wait()
        wbuf[w, f, block] = (gain_in[block] * w32[w, block]).astype(BF16)

    for i in order:
        for w in range(2):
            cast(w, i)
    pl.semaphore_wait(barrier, len(peers))

    def tok_copy(src, piece, slot, to):
        return remote(src, tbuf.at[piece], tok_s.at[slot], tok_r.at[piece], f, to)

    for slot, k in enumerate((1, 2, 4, 6)):
        tok_copy(tok_in, t, slot, flip(t, k)).start()

    def w_copy(w, src, i, sem, to):
        ref = wbuf.at[w, src, pl.ds(i * part, part)]
        return remote(ref, ref, sem, w_r.at[w, src, i], to, t)

    for step in range(CHUNKS):
        for w in range(2):
            w_copy(w, f, X_ORDER[step], own_s.at[0, w, X_ORDER[step]], fx).start()
            w_copy(w, f, Y_ORDER[step], own_s.at[1, w, Y_ORDER[step]], fy).start()

    def dz_copy(c, h):
        block = pl.ds(h * half, half)
        return remote(dcast.at[c, block], dbuf.at[t, block], dz_s.at[c, h], d_r.at[t, h], f, f * per + c)

    for c in range(per):
        load_down[c].wait()
        for h in range(2):
            block = pl.ds(h * half, half)
            dcast[c, block] = d32[pl.ds(c * tall + h * half, half)].astype(BF16)

        @pl.when(t == f * per + c)
        def _():
            dbuf[t] = dcast[c]

    for h in range(2):
        for c in range(per):
            @pl.when(t != f * per + c)
            def _():
                dz_copy(c, h).start()

    def store_w(w, src):
        return pltpu.make_async_copy(wbuf.at[w, src], w_outs[w].at[pl.ds(src * rows, rows)], out_w.at[w, src])

    for w in range(2):
        store_w(w, f).start()

    def arrive(step, w):
        i = X_ORDER[step]
        w_copy(w, fx, i, fwd_s.at[w, i], fy).wait_recv()
        if i < CHUNKS // 2:
            w_copy(w, fx, i, fwd_s.at[w, i], fy).start()
        i = Y_ORDER[step]
        w_copy(w, fy, i, fwd_s.at[w, i], fx).wait_recv()
        if i >= CHUNKS // 2:
            w_copy(w, fy, i, fwd_s.at[w, i], fx).start()

    tile = 256

    def accumulate(src, first):
        def one(n, _):
            w, column = n // (wbuf.shape[3] // tile), pl.multiple_of(n % (wbuf.shape[3] // tile) * tile, tile)
            total = 0.0 if first else acc[w, :, pl.ds(column, tile)]
            for p in range(per):
                total = total + jnp.dot(
                    tbuf[src * per + p],
                    wbuf[w, src, pl.ds(p * width, width), pl.ds(column, tile)],
                    preferred_element_type=F32,
                )
            acc[w, :, pl.ds(column, tile)] = total
            return 0

        lax.fori_loop(0, 2 * (wbuf.shape[3] // tile), one, 0)

    for step in range(CHUNKS // 2):
        for w in range(2):
            arrive(step, w)
    for slot, k in enumerate((2, 4, 6)):
        piece = flip(t, k)
        tok_copy(tok_in, piece, 4 + slot, mate).wait_recv()
        tok_copy(tbuf.at[piece], piece, 4 + slot, mate).start()
    for k in (1, 3, 5, 7):
        tok_copy(tok_in, flip(t, k), 0, mate).wait_recv()
    squares = jnp.zeros((n_tok, 1), F32)
    for p in range(n_tp):
        wide = tbuf[p].astype(F32)
        squares = squares + jnp.sum(wide * wide, axis=1, keepdims=True)
    scale[...] = lax.rsqrt(squares / (n_tp * width) + epsilon)
    accumulate(f, True)
    for step in range(CHUNKS // 2, CHUNKS):
        for w in range(2):
            arrive(step, w)
    for src in (fx, fy):
        for w in range(2):
            store_w(w, src).start()

    owner = t // per
    low, high = (f % 2 + owner % 2) % 2, (f // 2 + owner // 2) % 2
    is_source = f == owner
    to_first = fx + (fy - fx) * (low * (1 - high))
    to_second = fy + (fx - fy) * ((1 - low) * high)
    ends = ((1 - low) * high, low * (1 - high))
    nexts = (to_first, to_second)

    def d_copy(piece, h):
        ref = dbuf.at[piece, pl.ds(h * half, half)]
        return remote(ref, ref, d_s.at[piece, h], d_r.at[piece, h], nexts[h], t)

    def take(k):
        piece = flip(t, k)
        for h in range(2):
            @pl.when(jnp.logical_or(jnp.logical_not(is_source), k != 0))
            def _():
                d_copy(piece, h).wait_recv()

            @pl.when(ends[h] == 0)
            def _():
                d_copy(piece, h).start()

    @pl.when(is_source)
    def _():
        take(0)
        take(1)

    accumulate(fx, False)
    accumulate(fy, False)
    for i in (0, 2, 1, 3):
        for w in range(2):
            w_copy(w, fd, i, fwd_s.at[w, i], fx).wait_recv()
    for w in range(2):
        store_w(w, fd).start()
    accumulate(fd, False)

    def make_hidden(n, _):
        columns = pl.ds(pl.multiple_of(n * tile, tile), tile)
        s = scale[...]
        g = acc[0, :, columns] * s
        hidden[:, columns] = (g / (1.0 + jnp.exp(-g)) * (acc[1, :, columns] * s)).astype(BF16)
        return 0

    lax.fori_loop(0, hidden.shape[1] // tile, make_hidden, 0)

    def store_d(piece):
        columns = pl.ds(pl.multiple_of(piece * width, width), width)
        return pltpu.make_async_copy(dbuf.at[piece], down_out.at[:, columns], out_d.at[piece])

    def p_copy(k):
        return remote(psend.at[k], precv.at[k], p_s.at[k], p_r.at[k], f, mate)

    def z_copy(k, dz, piece):
        to = flip(t, 2 * dz)
        return remote(zsend.at[k, to // 2], zrecv.at[z, piece], z_s.at[k, dz], z_r.at[z, piece], f, to)

    def z_arrival(dz, piece):
        src = flip(t, 2 * dz)
        return remote(zsend.at[0, 0], zrecv.at[src // 2, piece], z_s.at[0, dz], z_r.at[src // 2, piece], f, src)

    n_z = n_tp // 2

    def finish(k):
        p_copy(k).wait_recv()
        for b in range(n_z):
            block = (keep[flip(k, 1), b] + precv[k, b].astype(F32)).astype(BF16)
            zsend[k, b] = block
        piece = flip(mate, k)
        zrecv[z, piece] = zsend[k, z]
        for dz in range(1, n_z):
            z_copy(k, dz, piece).start()

    def product(k):
        piece = flip(t, k)
        store_d(piece).start()
        out = jnp.dot(hidden[...], dbuf[piece], preferred_element_type=F32)
        out = out.reshape(n_z, 2, piece_rows, width)

        @pl.when(core == 0)
        def _():
            keep[k] = out[:, 0]
            psend[k] = out[:, 1].astype(BF16)

        @pl.when(core == 1)
        def _():
            keep[k] = out[:, 1]
            psend[k] = out[:, 0].astype(BF16)

        p_copy(k).start()

    def pair(i, _):
        for c in range(2):
            k = 2 * i + c

            @pl.when(jnp.logical_not(jnp.logical_and(is_source, i == 0)))
            def _():
                take(k)

            product(k)
        for c in range(2):
            finish(2 * i + c)
        return 0

    lax.fori_loop(0, n_tp // 2, pair, 0)

    for k in range(n_tp):
        for dz in range(1, n_z):
            z_arrival(dz, k).wait_recv()
    for piece in range(n_tp):
        total = zrecv[0, piece].astype(F32)
        for b in range(1, n_z):
            total = total + zrecv[b, piece].astype(F32)
        layer_out[:, pl.ds(piece * width, width)] = total.astype(BF16)

    for slot in range(4):
        tok_copy(tok_in, t, slot, mate).wait_send()
    for slot in range(3):
        tok_copy(tok_in, t, 4 + slot, mate).wait_send()
    for w in range(2):
        for i in range(CHUNKS):
            w_copy(w, f, i, own_s.at[0, w, i], fx).wait_send()
            w_copy(w, f, i, own_s.at[1, w, i], fy).wait_send()
            w_copy(w, f, i, fwd_s.at[w, i], fx).wait_send()
        for src in range(n_fs):
            store_w(w, src).wait()
    for c in range(per):
        for h in range(2):
            @pl.when(t != f * per + c)
            def _():
                dz_copy(c, h).wait_send()
    for k in range(n_tp):
        store_d(k).wait()
        p_copy(k).wait_send()
        for dz in range(1, n_z):
            z_copy(k, dz, k).wait_send()
        for h in range(2):
            @pl.when(ends[h] == 0)
            def _():
                d_copy(k, h).wait_send()


def body(tokens, norm_gain, gate_train, up_train, down_train, *, n_fs, n_tp):
    n_tok, width = tokens.shape
    rows, cols = gate_train.shape
    tall = down_train.shape[0] * n_fs // n_tp
    piece_rows = n_tok // n_tp
    n_z = n_tp // 2
    hbm = pl.BlockSpec(memory_space=pl.ANY)
    vmem = pl.BlockSpec(memory_space=pltpu.VMEM)
    dma = pltpu.SemaphoreType.DMA
    return pl.pallas_call(
        kernel,
        out_shape=(
            jax.ShapeDtypeStruct((rows * n_fs, cols), BF16),
            jax.ShapeDtypeStruct((rows * n_fs, cols), BF16),
            jax.ShapeDtypeStruct((tall, width * n_tp), BF16),
            jax.ShapeDtypeStruct((piece_rows, width * n_tp), BF16),
        ),
        in_specs=[vmem, vmem, hbm, hbm, hbm],
        out_specs=(hbm, hbm, hbm, vmem),
        scratch_shapes=[
            pltpu.VMEM((2, rows, cols), F32),
            pltpu.VMEM(down_train.shape, F32),
            pltpu.VMEM((2, n_fs, rows, cols), BF16),
            pltpu.VMEM((n_tp // n_fs, tall, width), BF16),
            pltpu.VMEM((n_tp, tall, width), BF16),
            pltpu.VMEM((n_tp, n_tok, width), BF16),
            pltpu.VMEM((2, n_tok, cols), F32),
            pltpu.VMEM((n_tok, cols), BF16),
            pltpu.VMEM((n_tok, 1), F32),
            pltpu.VMEM((n_tp, n_z, piece_rows, width), F32),
            pltpu.VMEM((n_tp, n_z, piece_rows, width), BF16),
            pltpu.VMEM((n_tp, n_z, piece_rows, width), BF16),
            pltpu.VMEM((n_tp, n_z, piece_rows, width), BF16),
            pltpu.VMEM((n_z, n_tp, piece_rows, width), BF16),
            dma((2, CHUNKS)),
            dma((n_tp // n_fs,)),
            dma((7,)),
            dma((n_tp,)),
            dma((2, 2, CHUNKS)),
            dma((2, CHUNKS)),
            dma((2, n_fs, CHUNKS)),
            dma((n_tp // n_fs, 2)),
            dma((n_tp, 2)),
            dma((n_tp, 2)),
            dma((2, n_fs)),
            dma((n_tp,)),
            dma((n_tp,)),
            dma((n_tp,)),
            dma((n_tp, n_z)),
            dma((n_z, n_tp)),
        ],
        compiler_params=pltpu.CompilerParams(
            collective_id=0, has_side_effects=True, vmem_limit_bytes=60 * 1024 * 1024
        ),
    )(tokens, norm_gain[:, None], gate_train, up_train, down_train)


def plain(tokens, norm_gain, gate_train, up_train, down_train):
    gate_local = (norm_gain[:, None] * gate_train).astype(BF16)
    up_local = (norm_gain[:, None] * up_train).astype(BF16)
    down_local = down_train.astype(BF16)
    features = lax.all_gather(tokens, "tp", axis=1, tiled=True)
    wide = features.astype(F32)
    squares = jnp.sum(wide * wide, axis=1)
    gate_whole = lax.all_gather(gate_local, "fs", axis=0, tiled=True)
    up_whole = lax.all_gather(up_local, "fs", axis=0, tiled=True)
    gate_sum = jnp.dot(features, gate_whole, preferred_element_type=F32)
    up_sum = jnp.dot(features, up_whole, preferred_element_type=F32)
    down_rows = lax.all_gather(down_local, "fs", axis=0, tiled=True)
    down_whole = lax.all_to_all(down_rows, "tp", split_axis=0, concat_axis=1, tiled=True)
    scale = lax.rsqrt(squares / features.shape[1] + epsilon)[:, None]
    hidden = (jax.nn.silu(gate_sum * scale) * (up_sum * scale)).astype(BF16)
    mixed = lax.psum_scatter(
        jnp.dot(hidden, down_whole, preferred_element_type=F32).astype(BF16), "tp", scatter_dimension=0, tiled=True
    )
    return (gate_whole, up_whole, down_whole, mixed)


def solution(mesh):
    n_fs, n_tp = mesh.shape["fs"], mesh.shape["tp"]
    fast = n_fs == 4 and n_tp == 8
    return jax.shard_map(
        functools.partial(body, n_fs=n_fs, n_tp=n_tp) if fast else plain,
        mesh=mesh,
        in_specs=(P("fs", "tp"), P("fs"), P("fs", "tp"), P("fs", "tp"), P("fs", "tp")),
        out_specs=(P(None, "tp"), P(None, "tp"), P("tp", None), P(("fs", "tp"), None)),
        check_vma=False,
    )
```

```python
import functools

import jax
import jax.numpy as jnp
from jax import lax
from jax.experimental import pallas as pl
from jax.experimental.pallas import tpu as pltpu
from jax.sharding import PartitionSpec as P

MESH = pl.DeviceIdType.MESH
BF16 = jnp.bfloat16
F32 = jnp.float32
epsilon = 1e-06
CHUNKS = 4
X_ORDER = (0, 1, 2, 3)
Y_ORDER = (2, 3, 0, 1)
QUARTERS = 4
LAG = 2


def flip(a, k):
    result = 0
    for bit in (1, 2, 4):
        own, other = (a // bit) % 2, (k // bit) % 2
        result = result + bit * (own + other - 2 * own * other)
    return result


def kernel(
    tok_in, gain_in, gate_in, up_in, down_in,
    gate_out, up_out, down_out, layer_out,
    w32, d32, wbuf, dcast, dbuf, tbuf, acc, hidden, scale, keep, psend, precv, zsend, zrecv,
    load_w, load_d, tok_s, tok_r, own_s, fwd_s, w_r, dz_s, d_s, d_r, out_w, out_d, p_s, p_r, z_s, z_r,
):
    f, t = lax.axis_index("fs"), lax.axis_index("tp")
    n_tp, n_fs = tbuf.shape[0], wbuf.shape[1]
    z, core = t // 2, t % 2
    fx, fy, fd = flip(f, 1), flip(f, 2), flip(f, 3)
    mate = flip(t, 1)
    rows = wbuf.shape[2]
    part = rows // CHUNKS
    w_ins, w_outs = (gate_in, up_in), (gate_out, up_out)
    tall, width = dbuf.shape[1], dbuf.shape[2]
    quarter = tall // QUARTERS
    per = n_tp // n_fs
    n_tok = tbuf.shape[1]
    piece_rows = n_tok // n_tp

    def remote(src, dst, ss, rs, to_f, to_t):
        return pltpu.make_async_remote_copy(
            src_ref=src, dst_ref=dst, send_sem=ss, recv_sem=rs, device_id=(to_f, to_t), device_id_type=MESH
        )

    def load(w, i):
        return pltpu.make_async_copy(w_ins[w].at[pl.ds(i * part, part)], w32.at[w, pl.ds(i * part, part)], load_w.at[w, i])

    order = (0, 2, 1, 3)
    for i in order:
        for w in range(2):
            load(w, i).start()
    load_down = [
        pltpu.make_async_copy(down_in.at[pl.ds(c * tall, tall)], d32.at[pl.ds(c * tall, tall)], load_d.at[c])
        for c in range(per)
    ]
    for copy in load_down:
        copy.start()

    barrier = pltpu.get_barrier_semaphore()
    peers = [(fx, t), (fy, t)] + [(f, flip(t, k)) for k in range(1, n_tp)]
    for peer in peers:
        pl.semaphore_signal(barrier, inc=1, device_id=peer, device_id_type=MESH)

    tbuf[t] = tok_in[...]

    def cast(w, i):
        block = pl.ds(i * part, part)
        load(w, i).wait()
        wbuf[w, f, block] = (gain_in[block] * w32[w, block]).astype(BF16)

    for i in order:
        for w in range(2):
            cast(w, i)
    pl.semaphore_wait(barrier, len(peers))

    def tok_copy(src, piece, slot, to):
        return remote(src, tbuf.at[piece], tok_s.at[slot], tok_r.at[piece], f, to)

    for slot, k in enumerate((1, 2, 4, 6)):
        tok_copy(tok_in, t, slot, flip(t, k)).start()

    def w_copy(w, src, i, sem, to):
        ref = wbuf.at[w, src, pl.ds(i * part, part)]
        return remote(ref, ref, sem, w_r.at[w, src, i], to, t)

    for step in range(CHUNKS):
        for w in range(2):
            w_copy(w, f, X_ORDER[step], own_s.at[0, w, X_ORDER[step]], fx).start()
            w_copy(w, f, Y_ORDER[step], own_s.at[1, w, Y_ORDER[step]], fy).start()

    def dz_copy(c, h):
        block = pl.ds(h * quarter, quarter)
        return remote(dcast.at[c, block], dbuf.at[t, block], dz_s.at[c, h], d_r.at[t, h], f, f * per + c)

    for c in range(per):
        load_down[c].wait()
        for h in range(QUARTERS):
            block = pl.ds(h * quarter, quarter)
            dcast[c, block] = d32[pl.ds(c * tall + h * quarter, quarter)].astype(BF16)

        @pl.when(t == f * per + c)
        def _():
            dbuf[t] = dcast[c]

    for h in range(QUARTERS):
        for c in range(per):
            @pl.when(t != f * per + c)
            def _():
                dz_copy(c, h).start()

    def store_w(w, src):
        return pltpu.make_async_copy(wbuf.at[w, src], w_outs[w].at[pl.ds(src * rows, rows)], out_w.at[w, src])

    for w in range(2):
        store_w(w, f).start()

    def arrive(step, w):
        i = X_ORDER[step]
        w_copy(w, fx, i, fwd_s.at[w, i], fy).wait_recv()
        if i < CHUNKS // 2:
            w_copy(w, fx, i, fwd_s.at[w, i], fy).start()
        i = Y_ORDER[step]
        w_copy(w, fy, i, fwd_s.at[w, i], fx).wait_recv()
        if i >= CHUNKS // 2:
            w_copy(w, fy, i, fwd_s.at[w, i], fx).start()

    tile = 512

    def accumulate(src, first):
        def one(n, _):
            w, column = n // (wbuf.shape[3] // tile), pl.multiple_of(n % (wbuf.shape[3] // tile) * tile, tile)
            total = 0.0 if first else acc[w, :, pl.ds(column, tile)]
            for p in range(per):
                total = total + jnp.dot(
                    tbuf[src * per + p],
                    wbuf[w, src, pl.ds(p * width, width), pl.ds(column, tile)],
                    preferred_element_type=F32,
                )
            acc[w, :, pl.ds(column, tile)] = total
            return 0

        lax.fori_loop(0, 2 * (wbuf.shape[3] // tile), one, 0)

    for step in range(CHUNKS // 2):
        for w in range(2):
            arrive(step, w)
    for slot, k in enumerate((2, 4, 6)):
        piece = flip(t, k)
        tok_copy(tok_in, piece, 4 + slot, mate).wait_recv()
        tok_copy(tbuf.at[piece], piece, 4 + slot, mate).start()
    for k in (1, 3, 5, 7):
        tok_copy(tok_in, flip(t, k), 0, mate).wait_recv()
    step_rows = n_tok // n_tp

    def norm(i, _):
        block = pl.ds(i * step_rows, step_rows)
        squares = 0.0
        for p in range(n_tp):
            wide = tbuf[p, block].astype(F32)
            squares = squares + wide * wide
        scale[block] = lax.rsqrt(jnp.sum(squares, axis=1, keepdims=True) / (n_tp * width) + epsilon)
        return 0

    lax.fori_loop(0, n_tp, norm, 0)
    accumulate(f, True)
    for step in range(CHUNKS // 2, CHUNKS):
        for w in range(2):
            arrive(step, w)
    for src in (fx, fy):
        for w in range(2):
            store_w(w, src).start()

    owner = t // per
    low, high = (f % 2 + owner % 2) % 2, (f // 2 + owner // 2) % 2
    is_source = f == owner
    to_first = fx + (fy - fx) * (low * (1 - high))
    to_second = fy + (fx - fy) * ((1 - low) * high)
    ends = ((1 - low) * high, low * (1 - high))
    nexts = (to_first, to_second)

    def d_copy(piece, h):
        ref = dbuf.at[piece, pl.ds(h * quarter, quarter)]
        return remote(ref, ref, d_s.at[piece, h], d_r.at[piece, h], nexts[h % 2], t)

    def pass_on(k):
        piece = flip(t, k)
        for h in range(QUARTERS):
            @pl.when(ends[h % 2] == 0)
            def _():
                if isinstance(k, int) and k == 0:
                    @pl.when(jnp.logical_not(is_source))
                    def _():
                        d_copy(piece, h).wait_recv()
                else:
                    d_copy(piece, h).wait_recv()
                d_copy(piece, h).start()

    def take_last(k):
        piece = flip(t, k)
        for h in range(QUARTERS):
            @pl.when(ends[h % 2] == 1)
            def _():
                d_copy(piece, h).wait_recv()

    @pl.when(is_source)
    def _():
        pass_on(0)
        pass_on(1)

    accumulate(fx, False)
    accumulate(fy, False)
    for i in (0, 2, 1, 3):
        for w in range(2):
            w_copy(w, fd, i, fwd_s.at[w, i], fx).wait_recv()
    for w in range(2):
        store_w(w, fd).start()
    accumulate(fd, False)

    @pl.when(jnp.logical_not(is_source))
    def _():
        pass_on(0)

    def make_hidden(n, _):
        columns = pl.ds(pl.multiple_of(n * tile, tile), tile)
        s = scale[...]
        g = acc[0, :, columns] * s
        hidden[:, columns] = (g / (1.0 + jnp.exp(-g)) * (acc[1, :, columns] * s)).astype(BF16)
        return 0

    lax.fori_loop(0, hidden.shape[1] // tile, make_hidden, 0)

    def store_d(piece):
        columns = pl.ds(pl.multiple_of(piece * width, width), width)
        return pltpu.make_async_copy(dbuf.at[piece], down_out.at[:, columns], out_d.at[piece])

    def p_copy(k):
        return remote(psend.at[k], precv.at[k], p_s.at[k], p_r.at[k], f, mate)

    def z_copy(k, dz, piece):
        to = flip(t, 2 * dz)
        return remote(zsend.at[k, to // 2], zrecv.at[z, piece], z_s.at[k, dz], z_r.at[z, piece], f, to)

    def z_arrival(dz, piece):
        src = flip(t, 2 * dz)
        return remote(zsend.at[0, 0], zrecv.at[src // 2, piece], z_s.at[0, dz], z_r.at[src // 2, piece], f, src)

    n_z = n_tp // 2

    def finish(k):
        p_copy(k).wait_recv()
        for b in range(n_z):
            block = (keep[flip(k, 1), b] + precv[k, b].astype(F32)).astype(BF16)
            zsend[k, b] = block
        piece = flip(mate, k)
        zrecv[z, piece] = zsend[k, z]
        for dz in range(1, n_z):
            z_copy(k, dz, piece).start()

    def product(k):
        piece = flip(t, k)
        store_d(piece).start()
        out = jnp.dot(hidden[...], dbuf[piece], preferred_element_type=F32)
        out = out.reshape(n_z, 2, piece_rows, width)

        @pl.when(core == 0)
        def _():
            keep[k] = out[:, 0]
            psend[k] = out[:, 1].astype(BF16)

        @pl.when(core == 1)
        def _():
            keep[k] = out[:, 1]
            psend[k] = out[:, 0].astype(BF16)

        p_copy(k).start()

    @pl.when(jnp.logical_not(is_source))
    def _():
        pass_on(1)

    def step(i, _):
        made, done = i, i - 2

        @pl.when(i + LAG < n_tp)
        def _():
            pass_on(i + LAG)

        @pl.when(made < n_tp)
        def _():
            take_last(made)
            product(made)

        @pl.when(done >= 0)
        def _():
            finish(done)

        return 0

    lax.fori_loop(0, n_tp + 2, step, 0)

    for k in range(n_tp):
        for dz in range(1, n_z):
            z_arrival(dz, k).wait_recv()
    for piece in range(n_tp):
        total = zrecv[0, piece].astype(F32)
        for b in range(1, n_z):
            total = total + zrecv[b, piece].astype(F32)
        layer_out[:, pl.ds(piece * width, width)] = total.astype(BF16)

    for slot in range(4):
        tok_copy(tok_in, t, slot, mate).wait_send()
    for slot in range(3):
        tok_copy(tok_in, t, 4 + slot, mate).wait_send()
    for w in range(2):
        for i in range(CHUNKS):
            w_copy(w, f, i, own_s.at[0, w, i], fx).wait_send()
            w_copy(w, f, i, own_s.at[1, w, i], fy).wait_send()
            w_copy(w, f, i, fwd_s.at[w, i], fx).wait_send()
        for src in range(n_fs):
            store_w(w, src).wait()
    for c in range(per):
        for h in range(QUARTERS):
            @pl.when(t != f * per + c)
            def _():
                dz_copy(c, h).wait_send()
    for k in range(n_tp):
        store_d(k).wait()
        p_copy(k).wait_send()
        for dz in range(1, n_z):
            z_copy(k, dz, k).wait_send()
        for h in range(QUARTERS):
            @pl.when(ends[h % 2] == 0)
            def _():
                d_copy(k, h).wait_send()


def body(tokens, norm_gain, gate_train, up_train, down_train, *, n_fs, n_tp):
    n_tok, width = tokens.shape
    rows, cols = gate_train.shape
    tall = down_train.shape[0] * n_fs // n_tp
    piece_rows = n_tok // n_tp
    n_z = n_tp // 2
    hbm = pl.BlockSpec(memory_space=pl.ANY)
    vmem = pl.BlockSpec(memory_space=pltpu.VMEM)
    dma = pltpu.SemaphoreType.DMA
    return pl.pallas_call(
        kernel,
        out_shape=(
            jax.ShapeDtypeStruct((rows * n_fs, cols), BF16),
            jax.ShapeDtypeStruct((rows * n_fs, cols), BF16),
            jax.ShapeDtypeStruct((tall, width * n_tp), BF16),
            jax.ShapeDtypeStruct((piece_rows, width * n_tp), BF16),
        ),
        in_specs=[vmem, vmem, hbm, hbm, hbm],
        out_specs=(hbm, hbm, hbm, vmem),
        scratch_shapes=[
            pltpu.VMEM((2, rows, cols), F32),
            pltpu.VMEM(down_train.shape, F32),
            pltpu.VMEM((2, n_fs, rows, cols), BF16),
            pltpu.VMEM((n_tp // n_fs, tall, width), BF16),
            pltpu.VMEM((n_tp, tall, width), BF16),
            pltpu.VMEM((n_tp, n_tok, width), BF16),
            pltpu.VMEM((2, n_tok, cols), F32),
            pltpu.VMEM((n_tok, cols), BF16),
            pltpu.VMEM((n_tok, 1), F32),
            pltpu.VMEM((n_tp, n_z, piece_rows, width), F32),
            pltpu.VMEM((n_tp, n_z, piece_rows, width), BF16),
            pltpu.VMEM((n_tp, n_z, piece_rows, width), BF16),
            pltpu.VMEM((n_tp, n_z, piece_rows, width), BF16),
            pltpu.VMEM((n_z, n_tp, piece_rows, width), BF16),
            dma((2, CHUNKS)),
            dma((n_tp // n_fs,)),
            dma((7,)),
            dma((n_tp,)),
            dma((2, 2, CHUNKS)),
            dma((2, CHUNKS)),
            dma((2, n_fs, CHUNKS)),
            dma((n_tp // n_fs, QUARTERS)),
            dma((n_tp, QUARTERS)),
            dma((n_tp, QUARTERS)),
            dma((2, n_fs)),
            dma((n_tp,)),
            dma((n_tp,)),
            dma((n_tp,)),
            dma((n_tp, n_z)),
            dma((n_z, n_tp)),
        ],
        compiler_params=pltpu.CompilerParams(
            collective_id=0, has_side_effects=True, vmem_limit_bytes=60 * 1024 * 1024
        ),
    )(tokens, norm_gain[:, None], gate_train, up_train, down_train)


def plain(tokens, norm_gain, gate_train, up_train, down_train):
    gate_local = (norm_gain[:, None] * gate_train).astype(BF16)
    up_local = (norm_gain[:, None] * up_train).astype(BF16)
    down_local = down_train.astype(BF16)
    features = lax.all_gather(tokens, "tp", axis=1, tiled=True)
    wide = features.astype(F32)
    squares = jnp.sum(wide * wide, axis=1)
    gate_whole = lax.all_gather(gate_local, "fs", axis=0, tiled=True)
    up_whole = lax.all_gather(up_local, "fs", axis=0, tiled=True)
    gate_sum = jnp.dot(features, gate_whole, preferred_element_type=F32)
    up_sum = jnp.dot(features, up_whole, preferred_element_type=F32)
    down_rows = lax.all_gather(down_local, "fs", axis=0, tiled=True)
    down_whole = lax.all_to_all(down_rows, "tp", split_axis=0, concat_axis=1, tiled=True)
    scale = lax.rsqrt(squares / features.shape[1] + epsilon)[:, None]
    hidden = (jax.nn.silu(gate_sum * scale) * (up_sum * scale)).astype(BF16)
    mixed = lax.psum_scatter(
        jnp.dot(hidden, down_whole, preferred_element_type=F32).astype(BF16), "tp", scatter_dimension=0, tiled=True
    )
    return (gate_whole, up_whole, down_whole, mixed)


def solution(mesh):
    n_fs, n_tp = mesh.shape["fs"], mesh.shape["tp"]
    fast = n_fs == 4 and n_tp == 8
    return jax.shard_map(
        functools.partial(body, n_fs=n_fs, n_tp=n_tp) if fast else plain,
        mesh=mesh,
        in_specs=(P("fs", "tp"), P("fs"), P("fs", "tp"), P("fs", "tp"), P("fs", "tp")),
        out_specs=(P(None, "tp"), P(None, "tp"), P("tp", None), P(("fs", "tp"), None)),
        check_vma=False,
    )
```
